128 devices in a mesh: sp: 16 (over z, x), dp: 8 (over y, core).
Axes of the slice: x: 4, y: 4, z: 4, core: 2. Of those that a mesh axis runs over, the one named last changes fastest.
Arguments:
- hidden_in: bfloat16 [8, 2048, 2048], P('dp', 'sp'), may hold values from -6 to 6
- mix_cotangent: bfloat16 [8, 2048, 4096], P('dp', 'sp'), may hold values from -0.119628906 to 0.119628906
- query_weight: bfloat16 [2048, 4096], P('dp', 'sp'), may hold values from -0.125 to 0.125
- key_weight: bfloat16 [2048, 4096], P('dp', 'sp'), may hold values from -0.125 to 0.125
- value_weight: bfloat16 [2048, 4096], P('dp', 'sp'), may hold values from -0.125 to 0.125
- decay_log: float32 [16], P('sp'), may hold values from -0.034 to -0.000146484375, as said below
Outputs:
- grad_hidden: bfloat16 [8, 2048, 2048], P('dp', 'sp')
- grad_query: float32 [2048, 4096], P('dp', 'sp')
- grad_key: float32 [2048, 4096], P('dp', 'sp')
- grad_value: float32 [2048, 4096], P('dp', 'sp')
The draws below stay inside these ranges and needn't reach their ends.
Inputs may be any that keep to these rules, and one draw needn't show every extreme that they name: Each head's decay_log is negative.
All inputs are finite; a program needn't handle non-finite values.
Results may differ from the reference program's by a relative error of at most 0.015.
Values may be sent and summed in bfloat16 or wider, within the bound.
A program may use at most 64 MiB of HBM per device.

```python
import jax
import jax.numpy as jnp
from jax import lax

D = 2048
HEADS = 16
BLOCK = 128
WIDTH = 4096
SEQ_LEN = 2048
SEQS = 8
N_SP = 16


def draw_decay_log(key, part):
    key_fast = jax.random.fold_in(key, 11)
    key_quick = jax.random.fold_in(key, 12)
    key_slow = jax.random.fold_in(key, 13)
    fast = jax.random.bernoulli(key_fast, 0.5, (HEADS,))
    quick_rate = jax.random.uniform(key_quick, (HEADS,), jnp.float32, 0.01, 0.034)
    slow_rate = jax.random.uniform(key_slow, (HEADS,), jnp.float32, 0.3, 2.0) / SEQ_LEN
    return -jnp.where(fast, quick_rate, slow_rate).astype(jnp.float32)


def block_levels(own_key, extent, cuts, smallest, largest):
    gain = 1.0
    for position, parts in cuts:
        heights = jax.random.uniform(jax.random.fold_in(jax.random.fold_in(own_key, 6), position), (parts,), jnp.float32, smallest / len(cuts), largest / len(cuts))
        gain = gain * jnp.repeat(jnp.exp(heights), extent[position] // parts).reshape((-1,) + (1,) * (len(extent) - 1 - position))
    return gain


def noise(rng, extent, scale, reach, split=(), kind=jnp.bfloat16):
    array = scale * jax.random.normal(rng, extent, jnp.float32)
    if split:
        array = array * block_levels(rng, extent, split, -0.22, 0.18)
    return jnp.clip(array, -reach, reach).astype(kind)


def setup_inputs(seed: int = 0) -> dict:
    seeds = jax.random.split(jax.random.key(seed), 7)
    return {
        "hidden_in": noise(seeds[0], (SEQS, SEQ_LEN, D), 1.0, 6.0, ((0, 8), (1, 16))),
        "mix_cotangent": noise(seeds[1], (SEQS, SEQ_LEN, WIDTH), 0.02, 0.119628906, ((0, 8), (1, 16))),
        "query_weight": noise(seeds[2], (D, WIDTH), D ** -0.5, 0.125, ((0, 8), (1, 16))),
        "key_weight": noise(seeds[3], (D, WIDTH), D ** -0.5, 0.125, ((0, 8), (1, 16))),
        "value_weight": noise(seeds[4], (D, WIDTH), D ** -0.5, 0.125, ((0, 8), (1, 16))),
        "decay_log": draw_decay_log(jax.random.fold_in(seeds[6], 71), 0),
    }


def head_grads(queries, key_rows, values, cotangent, log_rate):
    length = queries.shape[0]
    head_dim = queries.shape[1]
    blocks = length // BLOCK
    scale = head_dim ** -0.5
    keys_scaled = (key_rows.astype(jnp.float32) * scale).astype(jnp.bfloat16)
    offsets = jnp.arange(BLOCK, dtype=jnp.float32)
    spread = offsets[:, None] - offsets[None, :]
    inner_decay = jnp.where(spread >= 0, jnp.exp(log_rate * jnp.maximum(spread, 0.0)), 0.0)
    query_decay = jnp.exp(log_rate * (offsets + 1.0))
    key_decay = jnp.exp(log_rate * (BLOCK - 1.0 - offsets))
    block_decay = jnp.exp(log_rate * BLOCK)

    def split_blocks(series):
        return series.reshape(blocks, BLOCK, series.shape[-1])

    def forward(carried, inputs):
        query_block, key_block, value_block, grad_block = inputs
        mixed = (jnp.dot(grad_block, value_block.T, preferred_element_type=jnp.float32) * inner_decay).astype(jnp.bfloat16)
        within = jnp.dot(mixed, key_block, preferred_element_type=jnp.float32)
        across = jnp.dot(grad_block, carried.astype(jnp.bfloat16).T, preferred_element_type=jnp.float32) * query_decay[:, None]
        weighted = (key_block.astype(jnp.float32) * key_decay[:, None]).astype(jnp.bfloat16)
        updated = carried * block_decay + jnp.dot(weighted.T, value_block, preferred_element_type=jnp.float32)
        return updated, (within + across, mixed)

    def backward(carried, inputs):
        query_block, key_block, value_block, grad_block, mixed = inputs
        scores = (jnp.dot(query_block, key_block.T, preferred_element_type=jnp.float32) * inner_decay).astype(jnp.bfloat16)
        state_bf = carried.astype(jnp.bfloat16)
        grad_v = jnp.dot(scores.T, grad_block, preferred_element_type=jnp.float32) + jnp.dot(key_block, state_bf, preferred_element_type=jnp.float32) * key_decay[:, None]
        grad_k = (jnp.dot(mixed.T, query_block, preferred_element_type=jnp.float32) + jnp.dot(value_block, state_bf.T, preferred_element_type=jnp.float32) * key_decay[:, None]) * scale
        weighted = (query_block.astype(jnp.float32) * query_decay[:, None]).astype(jnp.bfloat16)
        updated = carried * block_decay + jnp.dot(weighted.T, grad_block, preferred_element_type=jnp.float32)
        return updated, (grad_k, grad_v)

    inputs = (split_blocks(queries), split_blocks(keys_scaled), split_blocks(values), split_blocks(cotangent))
    initial = jnp.zeros((head_dim, values.shape[-1]), jnp.float32)
    final_state, (grad_q, mixed_all) = lax.scan(forward, initial, inputs)
    final_back, (grad_k, grad_v) = lax.scan(backward, initial, inputs + (mixed_all,), reverse=True)
    return grad_q.reshape(length, -1), grad_k.reshape(length, -1), grad_v.reshape(length, -1)


def group_grads(log_rates, queries, key_rows, values, cotangent):
    length = queries.shape[0]
    head_count = log_rates.shape[0]

    def by_head(series):
        return series.reshape(length, head_count, -1).transpose(1, 0, 2)

    def to_rows(series):
        return series.transpose(1, 0, 2).reshape(length, -1)

    grad_q, grad_k, grad_v = jax.vmap(head_grads)(by_head(queries), by_head(key_rows), by_head(values), by_head(cotangent), log_rates)
    return jnp.concatenate((to_rows(grad_q), to_rows(grad_k), to_rows(grad_v)), axis=1).astype(jnp.bfloat16)


def reference(hidden_in, mix_cotangent, query_weight, key_weight, value_weight, decay_log):
    weights = jnp.concatenate((query_weight, key_weight, value_weight), axis=1)
    all_width = query_weight.shape[1]
    model_width = query_weight.shape[0]

    def one_sequence(seq_pair):
        seq_rows, seq_cotangent = seq_pair
        projected = jnp.dot(seq_rows, weights, preferred_element_type=jnp.float32).astype(jnp.bfloat16)
        gradients = group_grads(decay_log, projected[:, :all_width], projected[:, all_width:2 * all_width], projected[:, 2 * all_width:], seq_cotangent)
        length = seq_rows.shape[0]
        split_grads = gradients.reshape(length, 3, N_SP, -1).astype(jnp.float32)
        split_weights = weights.reshape(model_width, 3, N_SP, -1).astype(jnp.float32)
        partials = jnp.einsum('ltgc,dtgc->gld', split_grads, split_weights)
        rounded = lax.optimization_barrier(partials.astype(jnp.bfloat16)).astype(jnp.float32)
        return jnp.sum(rounded, axis=0).astype(jnp.bfloat16), gradients

    grad_hidden, all_grads = lax.map(one_sequence, (hidden_in, mix_cotangent))
    flat_rows = hidden_in.reshape(-1, model_width)
    flat_grads = all_grads.reshape(-1, 3 * all_width)
    summed = lax.dot_general(flat_rows, flat_grads, (((0,), (0,)), ((), ())), preferred_element_type=jnp.float32) / SEQS
    return grad_hidden, summed[:, :all_width], summed[:, all_width:2 * all_width], summed[:, 2 * all_width:]
```

```python
import jax
import jax.numpy as jnp
from jax import lax
from jax.experimental import pallas as pl
from jax.experimental.pallas import tpu as pltpu
from jax.sharding import PartitionSpec as P

BLOCK = 128


def in_blocks(array, dim, size):
    shape = array.shape
    pieces = array.reshape(*shape[:dim], size, shape[dim] // size, *shape[dim + 1 :])
    return jnp.moveaxis(pieces, dim, 0)


def sent_and_summed(array, axis, dim):
    pieces = in_blocks(array, dim, lax.axis_size(axis))
    arrived = lax.all_to_all(pieces, axis, split_axis=0, concat_axis=0, tiled=True)
    return arrived.astype(jnp.float32).sum(axis=0)


def dot(a, b, dims):
    return lax.dot_general(a, b, ((dims[:1], dims[1:]), ((), ())), preferred_element_type=jnp.float32)


def retention_kernel(rate_ref, qkv_ref, cot_ref, out_ref, inner, qdec, kdec, fstate, bstate):
    length = qkv_ref.shape[0]
    hd = cot_ref.shape[1]
    blocks = length // BLOCK
    scale = hd ** (-0.5)
    rate = rate_ref[0]
    row = lax.broadcasted_iota(jnp.int32, (BLOCK, BLOCK), 0).astype(jnp.float32)
    col = lax.broadcasted_iota(jnp.int32, (BLOCK, BLOCK), 1).astype(jnp.float32)
    spread = row - col
    inner[...] = jnp.where(spread >= 0, jnp.exp(rate * jnp.maximum(spread, 0.0)), 0.0)
    rows = lax.broadcasted_iota(jnp.int32, (BLOCK, hd), 0).astype(jnp.float32)
    qdec[...] = jnp.exp(rate * (rows + 1.0))
    kdec[...] = jnp.exp(rate * (BLOCK - 1.0 - rows))
    step_decay = jnp.exp(jnp.full((hd, hd), rate * BLOCK, jnp.float32))
    fstate[...] = jnp.zeros_like(fstate)
    bstate[...] = jnp.zeros_like(bstate)

    def load(n):
        at = pl.ds(pl.multiple_of(n * BLOCK, BLOCK), BLOCK)
        q = qkv_ref[at, 0:hd]
        k = (qkv_ref[at, hd : 2 * hd].astype(jnp.float32) * scale).astype(jnp.bfloat16)
        v = qkv_ref[at, 2 * hd : 3 * hd]
        c = cot_ref[at, :]
        return at, q, k, v, c

    def step(i, _):
        at, q, k, v, c = load(i)
        mixed = (dot(c, v, (1, 1)) * inner[...]).astype(jnp.bfloat16)
        s = fstate[...]
        gq = dot(mixed, k, (1, 0)) + dot(c, s.astype(jnp.bfloat16), (1, 0)) * qdec[...]
        out_ref[at, 0:hd] = gq.astype(jnp.bfloat16)
        kw = (k.astype(jnp.float32) * kdec[...]).astype(jnp.bfloat16)
        fstate[...] = s * step_decay + dot(v, kw, (0, 0))

        at, q, k, v, c = load(blocks - 1 - i)
        mixed = (dot(c, v, (1, 1)) * inner[...]).astype(jnp.bfloat16)
        scores = (dot(q, k, (1, 1)) * inner[...]).astype(jnp.bfloat16)
        r = bstate[...]
        rb = r.astype(jnp.bfloat16)
        gv = dot(scores, c, (0, 0)) + dot(k, rb, (1, 0)) * kdec[...]
        gk = (dot(mixed, q, (0, 0)) + dot(v, rb, (1, 1)) * kdec[...]) * scale
        out_ref[at, hd : 2 * hd] = gk.astype(jnp.bfloat16)
        out_ref[at, 2 * hd : 3 * hd] = gv.astype(jnp.bfloat16)
        qw = (q.astype(jnp.float32) * qdec[...]).astype(jnp.bfloat16)
        bstate[...] = r * step_decay + dot(qw, c, (0, 0))
        return 0

    lax.fori_loop(0, blocks, step, 0)


def retention(rate, qkv, cotangent):
    length, hd = cotangent.shape
    return pl.pallas_call(
        retention_kernel,
        out_shape=jax.ShapeDtypeStruct(qkv.shape, jnp.bfloat16),
        in_specs=[
            pl.BlockSpec(memory_space=pltpu.SMEM),
            pl.BlockSpec(memory_space=pltpu.VMEM),
            pl.BlockSpec(memory_space=pltpu.VMEM),
        ],
        out_specs=pl.BlockSpec(memory_space=pltpu.VMEM),
        scratch_shapes=[
            pltpu.VMEM((BLOCK, BLOCK), jnp.float32),
            pltpu.VMEM((BLOCK, hd), jnp.float32),
            pltpu.VMEM((BLOCK, hd), jnp.float32),
            pltpu.VMEM((hd, hd), jnp.float32),
            pltpu.VMEM((hd, hd), jnp.float32),
        ],
        cost_estimate=pl.CostEstimate(flops=2_000_000_000, bytes_accessed=8_000_000, transcendentals=0),
    )(rate, qkv, cotangent)


def body(hidden_in, mix_cotangent, query_weight, key_weight, value_weight, decay_log):
    own_rows = hidden_in[0]
    columns = query_weight.shape[1]
    stacked = jnp.stack((query_weight, key_weight, value_weight), axis=1)
    gathered = lax.all_gather(stacked, "dp", axis=0, tiled=True)
    weights = gathered.reshape(gathered.shape[0], 3 * columns)
    cotangent = lax.all_to_all(mix_cotangent[0], "sp", split_axis=1, concat_axis=0, tiled=True)
    all_rows = lax.all_gather(own_rows, "sp", axis=0, tiled=True)
    projected = jnp.dot(all_rows, weights, preferred_element_type=jnp.float32).astype(jnp.bfloat16)
    gradients = retention(decay_log, projected, cotangent)
    input_sum = lax.psum_scatter(
        lax.dot_general(
            gradients, weights, (((1,), (1,)), ((), ())), preferred_element_type=jnp.float32
        ).astype(jnp.bfloat16),
        "sp",
        scatter_dimension=0,
        tiled=True,
    )
    grad_hidden = input_sum[None]
    summed = sent_and_summed(
        lax.dot_general(
            all_rows, gradients, (((0,), (0,)), ((), ())), preferred_element_type=jnp.float32
        ).astype(jnp.bfloat16),
        "dp",
        0,
    ) / lax.axis_size("dp")
    return (
        grad_hidden,
        summed[:, :columns],
        summed[:, columns : 2 * columns],
        summed[:, 2 * columns :],
    )


def solution(mesh):
    placed = (
        P("dp", "sp", None),
        P("dp", "sp", None),
        P("dp", "sp"),
        P("dp", "sp"),
        P("dp", "sp"),
        P("sp"),
    )
    return jax.shard_map(
        body,
        mesh=mesh,
        in_specs=placed,
        out_specs=(P("dp", "sp", None), P("dp", "sp"), P("dp", "sp"), P("dp", "sp")),
        check_vma=False,
    )
```

```python
import jax
import jax.numpy as jnp
from jax import lax
from jax.experimental import pallas as pl
from jax.experimental.pallas import tpu as pltpu
from jax.sharding import PartitionSpec as P

BLOCK = 128
COPIES = 96
BF16 = jnp.bfloat16
F32 = jnp.float32


def dot(a, b, dims):
    return lax.dot_general(a, b, ((dims[:1], dims[1:]), ((), ())), preferred_element_type=F32)


def both(a, b):
    return (a.astype(F32) + b.astype(F32)).astype(BF16)


def offset(q):
    return jnp.where(q == 0, 2, jnp.where(q == 1, 1, jnp.where(q == 2, 3, 0)))


def kernel(
    rate_ref, hid, cot, wq, wk, wv,
    dx_out, dq_out, dk_out, dv_out,
    X, W, C, QKV, G, GT, PX, RB, EZ, FU, FD, SU, SD, EX, FIN, RFIN,
    DW, YFU, YFD, YSU, YSD, HB0, HB1, RT, PR, inner, qdec, kdec, sdec, fstate, bstate,
    ss, rs, csend, crecv, lsem,
):
    hd = wq.shape[1]
    depth = wq.shape[0]
    s = lax.axis_index("sp")
    d = lax.axis_index("dp")
    z, x = s // 4, s % 4
    y, c = d // 2, d % 2
    g = x // 2
    r = (c + g) % 2
    xp = x + 1 - 2 * (x % 2)
    j = z * 2 + x % 2
    up, down, far = (z + 1) % 4, (z + 3) % 4, (z + 2) % 4
    yu, yd, yf = (y + 1) % 4, (y + 3) % 4, (y + 2) % 4

    def at(zz, xx):
        return zz * 2 + xx % 2

    def dev(sp, dp):
        return {"sp": sp, "dp": dp}

    pair = dev(z * 4 + xp, d)
    zup, zdown = dev(up * 4 + x, d), dev(down * 4 + x, d)
    yup, ydown = dev(s, yu * 2 + c), dev(s, yd * 2 + c)
    sibling = dev(s, y * 2 + 1 - c)
    swap = z * 4 + 3 - x
    copies = {}

    def add(name, src, dst, device, landing=None):
        n = len(copies)
        copies[name] = pltpu.make_async_remote_copy(
            src_ref=src, dst_ref=dst, send_sem=ss.at[n], recv_sem=rs.at[n if landing is None else landing],
            device_id=device, device_id_type=pl.DeviceIdType.MESH,
        )

    def start(*names):
        for name in names:
            copies[name].start()

    def arrived(*names):
        for name in names:
            copies[name].wait_recv()

    half = BLOCK // 2
    quarter = BLOCK // 4
    xr, zr = pl.ds(0, half), pl.ds(half, half)

    def blk(zz, xx, rows):
        return X.at[2 * at(zz, xx) + r, rows]

    def ring(name, device, src):
        add(name, src, src, device)

    add("swap_x", hid.at[0], X.at[2 * at(z, 3 - x) + 1], dev(swap, y * 2 + 1 - c))
    ring("A", pair, blk(z, x, xr))
    for tag, xx, rows, o in (("z", x, zr, half), ("a", x, xr, 0), ("b", xp, xr, 0)):
        ring(tag + "u", zup, blk(z, xx, rows))
        ring(tag + "d", zdown, blk(z, xx, rows))
        ring(tag + "uu", zup, blk(down, xx, pl.ds(o, quarter)))
        ring(tag + "dd", zdown, blk(up, xx, pl.ds(o + quarter, quarter)))
    for tag, zz in (("H0", z), ("H1", down), ("H2", up), ("H3", far)):
        ring(tag, pair, blk(zz, x, zr))
    order = [(z, x), (down, x), (up, x), (far, x), (z, xp), (down, xp), (up, xp), (far, xp)]
    for n, (zz, xx) in enumerate(order):
        slot = X.at[2 * at(zz, xx) + r]
        add("D%d" % n, slot, slot, sibling)

    for n, w in enumerate((wq, wk, wv)):
        cols = pl.ds(n * hd, hd)
        add("own_w%d" % n, w, W.at[d, :, cols], sibling)
        add("swap_w%d" % n, w, W.at[d, :, cols], dev(swap, y * 2 + g), COPIES + 2 * n + c)
    for i in range(2):
        ring("wu%d" % i, yup, W.at[2 * y + i])
        ring("wd%d" % i, ydown, W.at[2 * y + i])
    ring("wuu", yup, W.at[2 * yd])
    ring("wdd", ydown, W.at[2 * yu + 1])
    add("rate", RT, PR, dev(swap, d))

    def out(zz, xx, rows):
        return RB.at[at(zz, xx), rows]

    porder = [(far, xp), (far, x), (up, xp), (up, x), (down, xp), (down, x), (z, xp), (z, x)]
    for n, (zz, xx) in enumerate(porder):
        add("P%d" % n, PX.at[2 * at(zz, xx) + 1 - r], RB.at[at(zz, xx)], sibling)
    for n, zz in enumerate((far, up, down, z)):
        add("EZ%d" % n, out(zz, xp, zr), EZ.at[zz], pair)
    cols3 = ((0, x, 0), (1, xp, 0), (2, x, half))
    for m, xx, o in cols3:
        add("FU%d" % m, out(far, xx, pl.ds(o, quarter)), FU.at[m], zup)
        add("FD%d" % m, out(far, xx, pl.ds(o + quarter, quarter)), FD.at[m], zdown)
        add("SU%d" % m, out(up, xx, pl.ds(o, half)), SU.at[m], zup)
        add("SD%d" % m, out(down, xx, pl.ds(o, half)), SD.at[m], zdown)
    add("EX", out(z, xp, xr), EX, pair)
    for n, rows in enumerate((xr, zr)):
        add("fin%d" % n, FIN.at[rows], RFIN.at[rows], dev(swap, y * 2 + 1 - c))

    add("YFU", DW.at[2 * yf], YFU, yup)
    add("YFD", DW.at[2 * yf + 1], YFD, ydown)
    for i in range(2):
        add("YSU%d" % i, DW.at[2 * yu + i], YSU.at[i], yup)
        add("YSD%d" % i, DW.at[2 * yd + i], YSD.at[i], ydown)
        add("hb1_%d" % i, DW.at[2 * y + i], HB1, dev(swap, 2 * y + i), COPIES + 6)
    add("hb0", DW.at[2 * y + 1 - c], HB0, sibling)

    RT[...] = jnp.full(RT.shape, rate_ref[0], F32)

    own_x = X.at[2 * j + r]
    local_x = pltpu.make_async_copy(hid.at[0], X.at[2 * j], rs.at[0])

    @pl.when(r == 0)
    def _():
        local_x.start()

    @pl.when(r == 1)
    def _():
        start("swap_x")

    for n, w in enumerate((wq, wk, wv)):
        start("swap_w%d" % n)

    @pl.when(r == 0)
    def _():
        for n, w in enumerate((wq, wk, wv)):
            pltpu.make_async_copy(w, W.at[d, :, pl.ds(n * hd, hd)], lsem.at[n]).start()

    @pl.when(r == 1)
    def _():
        for n in range(3):
            start("own_w%d" % n)

    pltpu.make_async_copy(own_x, own_x, rs.at[0]).wait()
    start("A", "zu", "zd", "H0", "au", "ad", "D0")

    bx = x + r * (3 - 2 * x)
    cslot = 2 * (z * 2 + bx - 2 * c) + r

    def cot_copy(k):
        h = (s + k) % 16
        hz, hx = h // 4, h % 4
        role = (hx // 2 + c) % 2
        tx = hx + role * (3 - 2 * hx)
        tc = c + role * (1 - 2 * c)
        src = cot.at[0, :, pl.ds(pl.multiple_of(h * hd, hd), hd)]
        same = jnp.logical_and(r == 0, k == 0)
        return same, src, dev(hz * 4 + tx, 2 * y + tc), csend.at[k]

    def cot_send(k, _):
        same, src, device, sem = cot_copy(k)

        @pl.when(same)
        def _():
            pltpu.make_async_copy(src, C.at[cslot], crecv).start()

        @pl.when(jnp.logical_not(same))
        def _():
            pltpu.make_async_remote_copy(
                src_ref=src, dst_ref=C.at[cslot], send_sem=sem, recv_sem=crecv,
                device_id=device, device_id_type=pl.DeviceIdType.MESH,
            ).start()

        return 0

    lax.fori_loop(0, 16, cot_send, 0)
    start("rate")

    arrived("A")
    start("bu", "bd")

    @pl.when(r == 0)
    def _():
        for n, w in enumerate((wq, wk, wv)):
            pltpu.make_async_copy(w, W.at[d, :, pl.ds(n * hd, hd)], lsem.at[n]).wait()
        arrived("own_w0", "own_w1", "own_w2")

    @pl.when(r == 1)
    def _():
        for n in range(3):
            for i in range(2):
                piece = W.at[2 * y + i, :, pl.ds(n * hd, hd)]
                pltpu.make_async_copy(piece, piece, rs.at[COPIES + 2 * n + i]).wait()

    start("wu0", "wd1", "wu1", "wd0")

    arrived("zu")
    start("zuu", "H1")
    arrived("zd")
    start("zdd", "H2")
    arrived("au")
    start("auu", "D1")
    arrived("ad")
    start("add", "D2")
    arrived("bu")
    start("buu")
    arrived("bd")
    start("bdd")
    arrived("zuu", "zdd")
    start("H3")
    arrived("wu0")
    start("wuu")
    arrived("wd1")
    start("wdd")
    arrived("auu", "add")
    start("D3")
    arrived("H0")
    start("D4")
    arrived("wu1", "wd0", "wuu", "wdd")

    def project(k, _):
        @pl.when(k == 3)
        def _():
            arrived("H1")
            start("D5")
            arrived("H2")
            start("D6")

        @pl.when(k == 6)
        def _():
            arrived("buu", "bdd", "H3")
            start("D7")

        for n in range(8):

            @pl.when(k == n)
            def _():
                arrived("D%d" % n)

        q = k % 4
        zz = (z + jnp.where(q == 0, 0, jnp.where(q == 1, 3, jnp.where(q == 2, 1, 2)))) % 4
        jj = at(zz, x + k // 4)
        rows = pl.ds(2 * jj, 2)
        a = X[rows].reshape(2 * BLOCK, X.shape[2])
        for n in range(3):
            b = W[:, :, n * hd : (n + 1) * hd].reshape(X.shape[2], hd)
            QKV[rows, :, n * hd : (n + 1) * hd] = dot(a, b, (1, 0)).astype(BF16).reshape(2, BLOCK, hd)
        return 0

    lax.fori_loop(0, 8, project, 0)

    arrived("rate")
    pltpu.make_async_copy(C, C, crecv).wait()
    rate = jnp.where(r == 0, RT[0:1, :], PR[0:1, :])
    row = lax.broadcasted_iota(jnp.int32, (BLOCK, BLOCK), 0).astype(F32)
    col = lax.broadcasted_iota(jnp.int32, (BLOCK, BLOCK), 1).astype(F32)
    spread = row - col
    inner[...] = jnp.where(spread >= 0, jnp.exp(rate * jnp.maximum(spread, 0.0)), 0.0)
    qd = jnp.exp(rate * (row + 1.0))
    kd = jnp.exp(rate * (BLOCK - 1.0 - row))
    qdec[...] = jnp.concatenate((qd, qd), axis=1)
    kdec[...] = jnp.concatenate((kd, kd), axis=1)
    sd = jnp.exp(rate * float(BLOCK))
    sdec[...] = jnp.concatenate((sd, sd), axis=1)
    fstate[...] = jnp.zeros_like(fstate)
    bstate[...] = jnp.zeros_like(bstate)
    scale = hd ** (-0.5)
    blocks = X.shape[0]

    def load(n):
        px = n % 4
        role = (px // 2 + g) % 2
        slot = 2 * at(n // 4, px + role * (3 - 2 * px)) + role
        q = QKV[slot, :, 0:hd]
        k = (QKV[slot, :, hd : 2 * hd].astype(F32) * scale).astype(BF16)
        v = QKV[slot, :, 2 * hd : 3 * hd]
        return slot, q, k, v, C[slot]

    def put(slot, n, value):
        value = value.astype(BF16)
        G[slot, :, n * hd : (n + 1) * hd] = value
        lanes = pl.ds(pl.multiple_of(slot * BLOCK, BLOCK), BLOCK)
        GT[n * hd : (n + 1) * hd, lanes] = value.T

    def retain(i, _):
        slot, q, k, v, ct = load(i)
        mixed = (dot(ct, v, (1, 1)) * inner[...]).astype(BF16)
        st = fstate[...]
        put(slot, 0, dot(mixed, k, (1, 0)) + dot(ct, st.astype(BF16), (1, 0)) * qdec[...])
        kw = (k.astype(F32) * kdec[...]).astype(BF16)
        fstate[...] = st * sdec[...] + dot(v, kw, (0, 0))

        slot, q, k, v, ct = load(blocks - 1 - i)
        mixed = (dot(ct, v, (1, 1)) * inner[...]).astype(BF16)
        scores = (dot(q, k, (1, 1)) * inner[...]).astype(BF16)
        st = bstate[...]
        sb = st.astype(BF16)
        put(slot, 1, (dot(mixed, q, (0, 0)) + dot(v, sb, (1, 1)) * kdec[...]) * scale)
        put(slot, 2, dot(scores, ct, (0, 0)) + dot(k, sb, (1, 0)) * kdec[...])
        qw = (q.astype(F32) * qdec[...]).astype(BF16)
        bstate[...] = st * sdec[...] + dot(qw, ct, (0, 0))
        return 0

    lax.fori_loop(0, blocks, retain, 0)

    def chip_sum(n):
        zz, xx = porder[n]
        arrived("P%d" % n)
        jj = at(zz, xx)
        RB[jj] = both(RB[jj], PX[2 * jj + r])

    def merge(ref, index, rows, other):
        ref[index, rows] = both(ref[index, rows], other)

    def ring_up(m):
        _, xx, o = cols3[m]
        arrived("FU%d" % m)
        merge(RB, at(up, xx), pl.ds(o, quarter), FU[m])
        start("SU%d" % m)

    def ring_down(m):
        _, xx, o = cols3[m]
        arrived("FD%d" % m)
        merge(RB, at(down, xx), pl.ds(o + quarter, quarter), FD[m])
        start("SD%d" % m)

    def pair_in(n):
        zz = (far, up, down, z)[n]
        arrived("EZ%d" % n)
        merge(RB, at(zz, x), zr, EZ[zz])

    def yblock(k):
        yo = jnp.where(k < 2, 2, jnp.where(k < 6, jnp.where(k % 2 == 0, 1, 3), 0))
        i = jnp.where(jnp.logical_or(k == 2, k == 3), (k + 1) % 2, k % 2)
        return 2 * ((y + yo) % 4) + i

    def products(k, _):
        jj = at((z + offset(k // 2)) % 4, x + 1 - k % 2)
        rows = pl.ds(2 * jj, 2)
        a = G[rows].reshape(2 * BLOCK, 3 * hd)
        for n in range(8):
            piece = dot(a, W[n], (1, 1)).astype(BF16)
            PX[rows, :, n * depth : (n + 1) * depth] = piece.reshape(2, BLOCK, depth)
        for n in range(8):

            @pl.when(k == n)
            def _():
                start("P%d" % n)

        db = yblock(k)
        cols = pl.ds(pl.multiple_of(db * depth, depth), depth)
        b = X[:, :, cols].reshape(blocks * BLOCK, depth)
        for n in range(3):
            part = pl.ds(n * hd, hd)
            DW[db, part, :] = dot(GT[part, :], b, (1, 0)).astype(BF16)

        @pl.when(k == 0)
        def _():
            start("YFU")
            chip_sum(0)
            start("EZ0", "FU1", "FD1")

        @pl.when(k == 1)
        def _():
            start("YFD")
            chip_sum(1)
            start("FU0", "FD0")

        @pl.when(k == 2)
        def _():
            start("YSU1")
            chip_sum(2)
            start("EZ1")

        @pl.when(k == 3)
        def _():
            start("YSD0")
            chip_sum(3)
            ring_up(1)

        @pl.when(k == 4)
        def _():
            chip_sum(4)
            start("EZ2")
            ring_down(1)
            ring_up(0)

        @pl.when(k == 5)
        def _():
            chip_sum(5)
            ring_down(0)
            pair_in(0)
            start("FU2", "FD2")
            arrived("YFU")
            DW[2 * yu] = both(DW[2 * yu], YFU[...])
            start("YSU0")

        @pl.when(k == 6)
        def _():
            arrived("YFD")
            DW[2 * yd + 1] = both(DW[2 * yd + 1], YFD[...])
            start("YSD1")
            chip_sum(6)
            start("EZ3")
            pair_in(1)
            ring_up(2)

        @pl.when(k == 7)
        def _():
            chip_sum(7)
            pair_in(2)
            ring_down(2)

        return 0

    lax.fori_loop(0, 8, products, 0)

    arrived("SU1", "SD1")
    jp = at(z, xp)
    RB[jp, xr] = (RB[jp, xr].astype(F32) + SU[1].astype(F32) + SD[1].astype(F32)).astype(BF16)
    start("EX")
    arrived("SU0", "SD0", "EX")
    total = RB[j, xr].astype(F32) + SU[0].astype(F32) + SD[0].astype(F32) + EX[...].astype(F32)
    FIN[xr] = total.astype(BF16)

    @pl.when(r == 1)
    def _():
        start("fin0")

    arrived("YSU1", "YSD0", "YSU0", "YSD1")
    for i in range(2):
        total = DW[2 * y + i].astype(F32) + YSU[i].astype(F32) + YSD[i].astype(F32)
        DW[2 * y + i] = total.astype(BF16)

    @pl.when(r == 0)
    def _():
        start("hb0")

    @pl.when(r == 1)
    def _():
        start("hb1_0", "hb1_1")

    pair_in(3)
    arrived("SU2", "SD2")
    total = RB[j, zr].astype(F32) + SU[2].astype(F32) + SD[2].astype(F32)
    FIN[zr] = total.astype(BF16)

    @pl.when(r == 0)
    def _():
        dx_out[0] = FIN[...]

    @pl.when(r == 1)
    def _():
        start("fin1")

    copies["hb1_0"].wait_recv()

    def weights_out(part):
        for n, ref in enumerate((dq_out, dk_out, dv_out)):
            rows = pl.ds(n * hd, hd)
            ref[...] = ((part[rows].astype(F32) + HB1[rows].astype(F32)) * 0.125).T

    @pl.when(r == 0)
    def _():
        weights_out(DW.at[2 * y + c])

    @pl.when(r == 1)
    def _():
        arrived("hb0")
        weights_out(HB0)
        arrived("fin0", "fin1")
        dx_out[0] = RFIN[...]

    only_one = ("swap_x", "own_w0", "own_w1", "own_w2", "fin0", "fin1", "hb1_0", "hb1_1")
    for name in copies:
        if name not in only_one and name != "hb0":
            copies[name].wait_send()

    @pl.when(r == 1)
    def _():
        for name in only_one:
            copies[name].wait_send()

    @pl.when(r == 0)
    def _():
        copies["hb0"].wait_send()

    def cot_done(k, _):
        same, src, device, sem = cot_copy(k)

        @pl.when(jnp.logical_not(same))
        def _():
            pltpu.make_async_remote_copy(
                src_ref=src, dst_ref=C.at[cslot], send_sem=sem, recv_sem=crecv,
                device_id=device, device_id_type=pl.DeviceIdType.MESH,
            ).wait_send()

        return 0

    lax.fori_loop(0, 16, cot_done, 0)


def body(hidden_in, mix_cotangent, query_weight, key_weight, value_weight, decay_log):
    model = hidden_in.shape[2]
    depth, hd = query_weight.shape
    ways = model // depth
    slots = 16
    vmem = pltpu.VMEM
    any_space = pl.BlockSpec(memory_space=pl.ANY)
    whole = pl.BlockSpec(memory_space=pltpu.VMEM)
    grad = jax.ShapeDtypeStruct((depth, hd), F32)
    return pl.pallas_call(
        kernel,
        out_shape=(jax.ShapeDtypeStruct(hidden_in.shape, BF16), grad, grad, grad),
        in_specs=[pl.BlockSpec(memory_space=pltpu.SMEM)] + [any_space] * 5,
        out_specs=(whole,) * 4,
        scratch_shapes=[
            vmem((slots, BLOCK, model), BF16),
            vmem((ways, depth, 3 * hd), BF16),
            vmem((slots, BLOCK, hd), BF16),
            vmem((slots, BLOCK, 3 * hd), BF16),
            vmem((slots, BLOCK, 3 * hd), BF16),
            vmem((3 * hd, slots * BLOCK), BF16),
            vmem((slots, BLOCK, model), BF16),
            vmem((slots // 2, BLOCK, model), BF16),
            vmem((4, BLOCK // 2, model), BF16),
            vmem((3, BLOCK // 4, model), BF16),
            vmem((3, BLOCK // 4, model), BF16),
            vmem((3, BLOCK // 2, model), BF16),
            vmem((3, BLOCK // 2, model), BF16),
            vmem((BLOCK // 2, model), BF16),
            vmem((BLOCK, model), BF16),
            vmem((BLOCK, model), BF16),
            vmem((ways, 3 * hd, depth), BF16),
            vmem((3 * hd, depth), BF16),
            vmem((3 * hd, depth), BF16),
            vmem((2, 3 * hd, depth), BF16),
            vmem((2, 3 * hd, depth), BF16),
            vmem((3 * hd, depth), BF16),
            vmem((3 * hd, depth), BF16),
            vmem((8, BLOCK), F32),
            vmem((8, BLOCK), F32),
            vmem((BLOCK, BLOCK), F32),
            vmem((BLOCK, hd), F32),
            vmem((BLOCK, hd), F32),
            vmem((1, hd), F32),
            vmem((hd, hd), F32),
            vmem((hd, hd), F32),
            pltpu.SemaphoreType.DMA((COPIES,)),
            pltpu.SemaphoreType.DMA((COPIES + 7,)),
            pltpu.SemaphoreType.DMA((16,)),
            pltpu.SemaphoreType.DMA,
            pltpu.SemaphoreType.DMA((3,)),
        ],
        compiler_params=pltpu.CompilerParams(has_side_effects=True, vmem_limit_bytes=60 * 1024 * 1024),
    )(decay_log, hidden_in, mix_cotangent, query_weight, key_weight, value_weight)


def solution(mesh):
    placed = (
        P("dp", "sp", None),
        P("dp", "sp", None),
        P("dp", "sp"),
        P("dp", "sp"),
        P("dp", "sp"),
        P("sp"),
    )
    return jax.shard_map(
        body,
        mesh=mesh,
        in_specs=placed,
        out_specs=(P("dp", "sp", None), P("dp", "sp"), P("dp", "sp"), P("dp", "sp")),
        check_vma=False,
    )
```

```python
import jax
import jax.numpy as jnp
from jax import lax
from jax.experimental import pallas as pl
from jax.experimental.pallas import tpu as pltpu
from jax.sharding import PartitionSpec as P

BLOCK = 128
COPIES = 96
BF16 = jnp.bfloat16
F32 = jnp.float32


def dot(a, b, dims):
    return lax.dot_general(a, b, ((dims[:1], dims[1:]), ((), ())), preferred_element_type=F32)


def both(a, b):
    return (a.astype(F32) + b.astype(F32)).astype(BF16)


def offset(q):
    return jnp.where(q == 0, 2, jnp.where(q == 1, 1, jnp.where(q == 2, 3, 0)))


def kernel(
    rate_ref, hid, cot, wq, wk, wv,
    dx_out, dq_out, dk_out, dv_out,
    X, W, C, QKV, G, GT, PX, RB, EZ, FU, FD, SU, SD, EX, FIN, RFIN,
    DW, YFU, YFD, YSU, YSD, HB0, HB1, RT, PR, inner, qdec, kdec, sdec, fstate, bstate,
    ss, rs, csend, crecv, lsem,
):
    hd = wq.shape[1]
    depth = wq.shape[0]
    s = lax.axis_index("sp")
    d = lax.axis_index("dp")
    z, x = s // 4, s % 4
    y, c = d // 2, d % 2
    g = x // 2
    r = (c + g) % 2
    xp = x + 1 - 2 * (x % 2)
    j = z * 2 + x % 2
    up, down, far = (z + 1) % 4, (z + 3) % 4, (z + 2) % 4
    yu, yd, yf = (y + 1) % 4, (y + 3) % 4, (y + 2) % 4

    def at(zz, xx):
        return zz * 2 + xx % 2

    def dev(sp, dp):
        return {"sp": sp, "dp": dp}

    pair = dev(z * 4 + xp, d)
    zup, zdown = dev(up * 4 + x, d), dev(down * 4 + x, d)
    yup, ydown = dev(s, yu * 2 + c), dev(s, yd * 2 + c)
    sibling = dev(s, y * 2 + 1 - c)
    swap = z * 4 + 3 - x
    copies = {}

    def add(name, src, dst, device, landing=None):
        n = len(copies)
        copies[name] = pltpu.make_async_remote_copy(
            src_ref=src, dst_ref=dst, send_sem=ss.at[n], recv_sem=rs.at[n if landing is None else landing],
            device_id=device, device_id_type=pl.DeviceIdType.MESH,
        )

    def start(*names):
        for name in names:
            copies[name].start()

    def arrived(*names):
        for name in names:
            copies[name].wait_recv()

    half = BLOCK // 2
    quarter = BLOCK // 4
    xr, zr = pl.ds(0, half), pl.ds(half, half)

    def blk(zz, xx, rows):
        return X.at[8 * r + at(zz, xx), rows]

    def ring(name, device, src):
        add(name, src, src, device)

    for n, rows in enumerate((xr, zr)):
        add("swap_x%d" % n, hid.at[0, rows], X.at[8 + at(z, 3 - x), rows], dev(swap, y * 2 + 1 - c))
    ring("A", pair, blk(z, x, xr))
    for tag, xx, rows, o in (("z", x, zr, half), ("a", x, xr, 0), ("b", xp, xr, 0)):
        ring(tag + "u", zup, blk(z, xx, rows))
        ring(tag + "d", zdown, blk(z, xx, rows))
        ring(tag + "uu", zup, blk(down, xx, pl.ds(o, quarter)))
        ring(tag + "dd", zdown, blk(up, xx, pl.ds(o + quarter, quarter)))
    for tag, zz in (("H0", z), ("H1", down), ("H2", up), ("H3", far)):
        ring(tag, pair, blk(zz, x, zr))
    order = [(z, x), (down, x), (up, x), (far, x), (z, xp), (down, xp), (up, xp), (far, xp)]
    for n, (zz, xx) in enumerate(order):
        slot = X.at[8 * r + at(zz, xx)]
        add("D%d" % n, slot, slot, sibling)

    for n, w in enumerate((wq, wk, wv)):
        cols = pl.ds(n * hd, hd)
        add("own_w%d" % n, w, W.at[d, :, cols], sibling)
        add("swap_w%d" % n, w, W.at[d, :, cols], dev(swap, y * 2 + g), COPIES + 2 * n + c)
    for i in range(2):
        ring("wu%d" % i, yup, W.at[2 * y + i])
        ring("wd%d" % i, ydown, W.at[2 * y + i])
    ring("wuu", yup, W.at[2 * yd])
    ring("wdd", ydown, W.at[2 * yu + 1])
    add("rate", RT, PR, dev(swap, d))

    def out(zz, xx, rows):
        return RB.at[at(zz, xx), rows]

    zorder = (far, up, down, z)
    for n, zz in enumerate(zorder):
        add("P%d" % n, PX.at[pl.ds(8 * (1 - r) + 2 * zz, 2)], RB.at[pl.ds(2 * zz, 2)], sibling)
    for n, zz in enumerate((far, up, down, z)):
        add("EZ%d" % n, out(zz, xp, zr), EZ.at[zz], pair)
    cols3 = ((0, x, 0), (1, xp, 0), (2, x, half))
    for m, xx, o in cols3:
        add("FU%d" % m, out(far, xx, pl.ds(o, quarter)), FU.at[m], zup)
        add("FD%d" % m, out(far, xx, pl.ds(o + quarter, quarter)), FD.at[m], zdown)
        add("SU%d" % m, out(up, xx, pl.ds(o, half)), SU.at[m], zup)
        add("SD%d" % m, out(down, xx, pl.ds(o, half)), SD.at[m], zdown)
    add("EX", out(z, xp, xr), EX, pair)
    for n, rows in enumerate((xr, zr)):
        add("fin%d" % n, FIN.at[rows], RFIN.at[rows], dev(swap, y * 2 + 1 - c))

    add("YFU", DW.at[2 * yf], YFU, yup)
    add("YFD", DW.at[2 * yf + 1], YFD, ydown)
    for i in range(2):
        add("YSU%d" % i, DW.at[2 * yu + i], YSU.at[i], yup)
        add("YSD%d" % i, DW.at[2 * yd + i], YSD.at[i], ydown)
        add("hb1_%d" % i, DW.at[2 * y + i], HB1, dev(swap, 2 * y + i), COPIES + 6)
    add("hb0", DW.at[2 * y + 1 - c], HB0, sibling)

    barrier = pltpu.get_barrier_semaphore()

    def greet(k, _):
        pl.semaphore_signal(
            barrier, inc=1, device_id=dev((s + k // 2) % 16, 2 * y + (c + k) % 2),
            device_id_type=pl.DeviceIdType.MESH,
        )
        return 0

    for device in (yup, ydown):
        pl.semaphore_signal(barrier, inc=1, device_id=device, device_id_type=pl.DeviceIdType.MESH)
    lax.fori_loop(1, 32, greet, 0)

    def local_weights():
        return [
            pltpu.make_async_copy(w, W.at[d, :, pl.ds(n * hd, hd)], lsem.at[n])
            for n, w in enumerate((wq, wk, wv))
        ]

    @pl.when(r == 0)
    def _():
        for n, rows in enumerate((xr, zr)):
            pltpu.make_async_copy(hid.at[0, rows], X.at[j, rows], rs.at[n]).start()
        for copy in local_weights():
            copy.start()

    RT[...] = jnp.full(RT.shape, rate_ref[0], F32)
    pl.semaphore_wait(barrier, 33)

    bx = x + r * (3 - 2 * x)
    cslot = 8 * r + z * 2 + bx - 2 * c

    def cot_copy(k):
        h = (s + k) % 16
        hz, hx = h // 4, h % 4
        role = (hx // 2 + c) % 2
        tx = hx + role * (3 - 2 * hx)
        tc = c + role * (1 - 2 * c)
        src = cot.at[0, :, pl.ds(pl.multiple_of(h * hd, hd), hd)]
        same = jnp.logical_and(r == 0, k == 0)
        return same, src, dev(hz * 4 + tx, 2 * y + tc), csend.at[k]

    def cot_send(k, _):
        same, src, device, sem = cot_copy(k)

        @pl.when(same)
        def _():
            pltpu.make_async_copy(src, C.at[cslot], crecv).start()

        @pl.when(jnp.logical_not(same))
        def _():
            pltpu.make_async_remote_copy(
                src_ref=src, dst_ref=C.at[cslot], send_sem=sem, recv_sem=crecv,
                device_id=device, device_id_type=pl.DeviceIdType.MESH,
            ).start()

        return 0

    def wait_own(n, rows):
        own = X.at[8 * r + j, rows]
        pltpu.make_async_copy(own, own, rs.at[n]).wait()

    def late_a():
        arrived("H1")
        start("D5")
        arrived("H2")
        start("D6")

    def late_b():
        arrived("buu", "bdd", "H3")
        start("D7")

    @pl.when(r == 1)
    def _():
        start("swap_x0", "swap_x1")
        for n in range(3):
            start("own_w%d" % n)
        for n in range(3):
            start("swap_w%d" % n)
        lax.fori_loop(0, 16, cot_send, 0)

    wait_own(0, xr)
    start("A", "au", "ad")
    wait_own(1, zr)
    start("zu", "zd", "H0", "D0")

    @pl.when(r == 0)
    def _():
        for copy in local_weights():
            copy.wait()
        arrived("own_w0", "own_w1", "own_w2")
        start("wu0", "wd1", "wu1", "wd0")

    start("rate")
    arrived("A")
    start("bu", "bd")

    @pl.when(r == 0)
    def _():
        for n in range(3):
            start("swap_w%d" % n)

    @pl.when(r == 1)
    def _():
        for n in range(3):
            for i in range(2):
                piece = W.at[2 * y + i, :, pl.ds(n * hd, hd)]
                pltpu.make_async_copy(piece, piece, rs.at[COPIES + 2 * n + i]).wait()
        start("wu0", "wd1", "wu1", "wd0")

    arrived("au")
    start("auu")
    arrived("ad")
    start("add")
    arrived("zu")
    start("zuu", "H1", "D1")
    arrived("zd")
    start("zdd", "H2", "D2")

    def forward_weights():
        arrived("wu0")
        start("wuu")
        arrived("wd1")
        start("wdd")

    @pl.when(r == 0)
    def _():
        forward_weights()

    arrived("bu")
    start("buu")
    arrived("bd")
    start("bdd")

    @pl.when(r == 0)
    def _():
        lax.fori_loop(0, 16, cot_send, 0)

    arrived("zuu", "zdd")
    start("H3")

    @pl.when(r == 1)
    def _():
        forward_weights()

    arrived("auu", "add")
    start("D3")
    arrived("H0")
    start("D4")

    @pl.when(r == 0)
    def _():
        late_a()
        late_b()

    arrived("wu1", "wd0", "wuu", "wdd")

    def project(k, _):
        @pl.when(jnp.logical_and(r == 1, k == 4))
        def _():
            late_a()

        @pl.when(jnp.logical_and(r == 1, k == 6))
        def _():
            late_b()

        for n in range(4):

            @pl.when(k == n + 4 * (1 - r))
            def _():
                arrived("D%d" % n, "D%d" % (n + 4))

        q = k % 4
        zz = (z + jnp.where(q == 0, 0, jnp.where(q == 1, 3, jnp.where(q == 2, 1, 2)))) % 4
        rows = pl.ds(8 * (k // 4) + 2 * zz, 2)
        a = X[rows].reshape(2 * BLOCK, X.shape[2])
        for n in range(3):
            b = W[:, :, n * hd : (n + 1) * hd].reshape(X.shape[2], hd)
            QKV[rows, :, n * hd : (n + 1) * hd] = dot(a, b, (1, 0)).astype(BF16).reshape(2, BLOCK, hd)
        return 0

    lax.fori_loop(0, 8, project, 0)

    arrived("rate")
    pltpu.make_async_copy(C, C, crecv).wait()
    rate = jnp.where(r == 0, RT[0:1, :], PR[0:1, :])
    row = lax.broadcasted_iota(jnp.int32, (BLOCK, BLOCK), 0).astype(F32)
    col = lax.broadcasted_iota(jnp.int32, (BLOCK, BLOCK), 1).astype(F32)
    spread = row - col
    inner[...] = jnp.where(spread >= 0, jnp.exp(rate * jnp.maximum(spread, 0.0)), 0.0)
    qd = jnp.exp(rate * (row + 1.0))
    kd = jnp.exp(rate * (BLOCK - 1.0 - row))
    qdec[...] = jnp.concatenate((qd, qd), axis=1)
    kdec[...] = jnp.concatenate((kd, kd), axis=1)
    sd = jnp.exp(rate * float(BLOCK))
    sdec[...] = jnp.concatenate((sd, sd), axis=1)
    fstate[...] = jnp.zeros_like(fstate)
    bstate[...] = jnp.zeros_like(bstate)
    scale = hd ** (-0.5)
    blocks = X.shape[0]

    def load(n):
        px = n % 4
        role = (px // 2 + g) % 2
        slot = 8 * role + at(n // 4, px + role * (3 - 2 * px))
        q = QKV[slot, :, 0:hd]
        k = (QKV[slot, :, hd : 2 * hd].astype(F32) * scale).astype(BF16)
        v = QKV[slot, :, 2 * hd : 3 * hd]
        return slot, q, k, v, C[slot]

    def put(slot, n, value):
        value = value.astype(BF16)
        G[slot, :, n * hd : (n + 1) * hd] = value
        lanes = pl.ds(pl.multiple_of(slot * BLOCK, BLOCK), BLOCK)
        GT[n * hd : (n + 1) * hd, lanes] = value.T

    def retain(i, _):
        slot, q, k, v, ct = load(i)
        mixed = (dot(ct, v, (1, 1)) * inner[...]).astype(BF16)
        st = fstate[...]
        put(slot, 0, dot(mixed, k, (1, 0)) + dot(ct, st.astype(BF16), (1, 0)) * qdec[...])
        kw = (k.astype(F32) * kdec[...]).astype(BF16)
        fstate[...] = st * sdec[...] + dot(v, kw, (0, 0))

        slot, q, k, v, ct = load(blocks - 1 - i)
        mixed = (dot(ct, v, (1, 1)) * inner[...]).astype(BF16)
        scores = (dot(q, k, (1, 1)) * inner[...]).astype(BF16)
        st = bstate[...]
        sb = st.astype(BF16)
        put(slot, 1, (dot(mixed, q, (0, 0)) + dot(v, sb, (1, 1)) * kdec[...]) * scale)
        put(slot, 2, dot(scores, ct, (0, 0)) + dot(k, sb, (1, 0)) * kdec[...])
        qw = (q.astype(F32) * qdec[...]).astype(BF16)
        bstate[...] = st * sdec[...] + dot(qw, ct, (0, 0))
        return 0

    lax.fori_loop(0, blocks, retain, 0)

    def chip_sum(n):
        zz = zorder[n]
        arrived("P%d" % n)
        for xx, names in ((xp, ("EZ%d" % n, "FU1", "FD1")), (x, ("FU0", "FD0"))):
            jj = at(zz, xx)
            RB[jj] = both(RB[jj], PX[8 * r + jj])
            if n:
                names = tuple(name for name in names if name[0] == "E")
            start(*names)

    def merge(ref, index, rows, other):
        ref[index, rows] = both(ref[index, rows], other)

    def ring_up(m):
        _, xx, o = cols3[m]
        arrived("FU%d" % m)
        merge(RB, at(up, xx), pl.ds(o, quarter), FU[m])
        start("SU%d" % m)

    def ring_down(m):
        _, xx, o = cols3[m]
        arrived("FD%d" % m)
        merge(RB, at(down, xx), pl.ds(o + quarter, quarter), FD[m])
        start("SD%d" % m)

    def pair_in(n):
        zz = (far, up, down, z)[n]
        arrived("EZ%d" % n)
        merge(RB, at(zz, x), zr, EZ[zz])

    def yblock(k):
        yo = jnp.where(k < 2, 2, jnp.where(k < 6, jnp.where(k % 2 == 0, 1, 3), 0))
        i = jnp.where(jnp.logical_or(k == 2, k == 3), (k + 1) % 2, k % 2)
        return 2 * ((y + yo) % 4) + i

    def weights_product(k):
        db = yblock(k)
        cols = pl.ds(pl.multiple_of(db * depth, depth), depth)
        b = X[:, :, cols].reshape(blocks * BLOCK, depth)
        for n in range(3):
            part = pl.ds(n * hd, hd)
            DW[db, part, :] = dot(GT[part, :], b, (1, 0)).astype(BF16)

    def products(k, _):
        weights_product(k)
        for n, names in enumerate((("YFU",), ("YFD",), ("YSU1",), ("YSD0",))):

            @pl.when(k == n)
            def _():
                start(*names)

        q = k // 2
        zz = (z + offset(q)) % 4
        rows = pl.ds(8 * ((1 - r + k) % 2) + 2 * zz, 2)
        a = G[rows].reshape(2 * BLOCK, 3 * hd)
        for n in range(8):
            piece = dot(a, W[n], (1, 1)).astype(BF16)
            PX[rows, :, n * depth : (n + 1) * depth] = piece.reshape(2, BLOCK, depth)
        for n in range(4):

            @pl.when(k == 2 * n)
            def _():
                start("P%d" % n)

            @pl.when(k == 2 * n + 1)
            def _():
                chip_sum(n)

        @pl.when(k == 4)
        def _():
            ring_up(1)
            ring_up(0)
            arrived("YFU")
            DW[2 * yu] = both(DW[2 * yu], YFU[...])
            start("YSU0")

        @pl.when(k == 5)
        def _():
            ring_down(1)
            ring_down(0)
            pair_in(0)
            start("FU2", "FD2")
            arrived("YFD")
            DW[2 * yd + 1] = both(DW[2 * yd + 1], YFD[...])
            start("YSD1")

        return 0

    lax.fori_loop(0, 8, products, 0)

    jp = at(z, xp)
    arrived("SU1", "SD1")
    RB[jp, xr] = (RB[jp, xr].astype(F32) + SU[1].astype(F32) + SD[1].astype(F32)).astype(BF16)
    start("EX")
    pair_in(1)
    ring_up(2)
    pair_in(2)
    ring_down(2)

    for i in range(2):
        arrived("YSU%d" % i, "YSD%d" % i)
        total = DW[2 * y + i].astype(F32) + YSU[i].astype(F32) + YSD[i].astype(F32)
        DW[2 * y + i] = total.astype(BF16)

        @pl.when(r == 1)
        def _():
            start("hb1_%d" % i)

    @pl.when(r == 0)
    def _():
        start("hb0")

    arrived("SU0", "SD0", "EX")
    total = RB[j, xr].astype(F32) + SU[0].astype(F32) + SD[0].astype(F32) + EX[...].astype(F32)
    FIN[xr] = total.astype(BF16)

    @pl.when(r == 1)
    def _():
        start("fin0")

    pair_in(3)
    arrived("SU2", "SD2")
    total = RB[j, zr].astype(F32) + SU[2].astype(F32) + SD[2].astype(F32)
    FIN[zr] = total.astype(BF16)

    @pl.when(r == 0)
    def _():
        dx_out[0] = FIN[...]

    @pl.when(r == 1)
    def _():
        start("fin1")

    copies["hb1_0"].wait_recv()

    def weights_out(part):
        for n, ref in enumerate((dq_out, dk_out, dv_out)):
            rows = pl.ds(n * hd, hd)
            ref[...] = ((part[rows].astype(F32) + HB1[rows].astype(F32)) * 0.125).T

    @pl.when(r == 0)
    def _():
        weights_out(DW.at[2 * y + c])

    @pl.when(r == 1)
    def _():
        arrived("hb0")
        weights_out(HB0)
        arrived("fin0", "fin1")
        dx_out[0] = RFIN[...]

    only_one = ("swap_x0", "swap_x1", "own_w0", "own_w1", "own_w2", "fin0", "fin1", "hb1_0", "hb1_1")
    for name in copies:
        if name not in only_one and name != "hb0":
            copies[name].wait_send()

    @pl.when(r == 1)
    def _():
        for name in only_one:
            copies[name].wait_send()

    @pl.when(r == 0)
    def _():
        copies["hb0"].wait_send()

    def cot_done(k, _):
        same, src, device, sem = cot_copy(k)

        @pl.when(jnp.logical_not(same))
        def _():
            pltpu.make_async_remote_copy(
                src_ref=src, dst_ref=C.at[cslot], send_sem=sem, recv_sem=crecv,
                device_id=device, device_id_type=pl.DeviceIdType.MESH,
            ).wait_send()

        return 0

    lax.fori_loop(0, 16, cot_done, 0)


def hand_over(*refs):
    n = len(refs) // 2
    pairs = [pltpu.make_async_copy(refs[i], refs[n + i], refs[-1].at[i]) for i in range(n)]
    for copy in pairs:
        copy.start()
    for copy in pairs:
        copy.wait()


def body(hidden_in, mix_cotangent, query_weight, key_weight, value_weight, decay_log):
    model = hidden_in.shape[2]
    depth, hd = query_weight.shape
    ways = model // depth
    slots = 16
    vmem = pltpu.VMEM
    any_space = pl.BlockSpec(memory_space=pl.ANY)
    far_space = pl.BlockSpec(memory_space=pltpu.HBM)
    whole = pl.BlockSpec(memory_space=pltpu.VMEM)
    grad = jax.ShapeDtypeStruct((depth, hd), F32)
    results = pl.pallas_call(
        kernel,
        out_shape=(jax.ShapeDtypeStruct(hidden_in.shape, BF16), grad, grad, grad),
        in_specs=[pl.BlockSpec(memory_space=pltpu.SMEM)] + [far_space] * 5,
        out_specs=(whole,) * 4,
        scratch_shapes=[
            vmem((slots, BLOCK, model), BF16),
            vmem((ways, depth, 3 * hd), BF16),
            vmem((slots, BLOCK, hd), BF16),
            vmem((slots, BLOCK, 3 * hd), BF16),
            vmem((slots, BLOCK, 3 * hd), BF16),
            vmem((3 * hd, slots * BLOCK), BF16),
            vmem((slots, BLOCK, model), BF16),
            vmem((slots // 2, BLOCK, model), BF16),
            vmem((4, BLOCK // 2, model), BF16),
            vmem((3, BLOCK // 4, model), BF16),
            vmem((3, BLOCK // 4, model), BF16),
            vmem((3, BLOCK // 2, model), BF16),
            vmem((3, BLOCK // 2, model), BF16),
            vmem((BLOCK // 2, model), BF16),
            vmem((BLOCK, model), BF16),
            vmem((BLOCK, model), BF16),
            vmem((ways, 3 * hd, depth), BF16),
            vmem((3 * hd, depth), BF16),
            vmem((3 * hd, depth), BF16),
            vmem((2, 3 * hd, depth), BF16),
            vmem((2, 3 * hd, depth), BF16),
            vmem((3 * hd, depth), BF16),
            vmem((3 * hd, depth), BF16),
            vmem((8, BLOCK), F32),
            vmem((8, BLOCK), F32),
            vmem((BLOCK, BLOCK), F32),
            vmem((BLOCK, hd), F32),
            vmem((BLOCK, hd), F32),
            vmem((1, hd), F32),
            vmem((hd, hd), F32),
            vmem((hd, hd), F32),
            pltpu.SemaphoreType.DMA((COPIES,)),
            pltpu.SemaphoreType.DMA((COPIES + 7,)),
            pltpu.SemaphoreType.DMA((16,)),
            pltpu.SemaphoreType.DMA,
            pltpu.SemaphoreType.DMA((3,)),
        ],
        compiler_params=pltpu.CompilerParams(collective_id=0, has_side_effects=True, vmem_limit_bytes=52 * 1024 * 1024),
    )(decay_log, hidden_in, mix_cotangent, query_weight, key_weight, value_weight)
    return pl.pallas_call(
        hand_over,
        out_shape=(jax.ShapeDtypeStruct(hidden_in.shape, BF16), grad, grad, grad),
        in_specs=[any_space] * 4,
        out_specs=(any_space,) * 4,
        scratch_shapes=[pltpu.SemaphoreType.DMA((4,))],
        compiler_params=pltpu.CompilerParams(vmem_limit_bytes=1024 * 1024),
    )(*results)


def solution(mesh):
    placed = (
        P("dp", "sp", None),
        P("dp", "sp", None),
        P("dp", "sp"),
        P("dp", "sp"),
        P("dp", "sp"),
        P("sp"),
    )
    return jax.shard_map(
        body,
        mesh=mesh,
        in_specs=placed,
        out_specs=(P("dp", "sp", None), P("dp", "sp"), P("dp", "sp"), P("dp", "sp")),
        check_vma=False,
    )
```

```python
import jax
import jax.numpy as jnp
from jax import lax
from jax.experimental import pallas as pl
from jax.experimental.pallas import tpu as pltpu
from jax.sharding import PartitionSpec as P

BLOCK = 128
COPIES = 128
BF16 = jnp.bfloat16
F32 = jnp.float32


def dot(a, b, dims):
    return lax.dot_general(a, b, ((dims[:1], dims[1:]), ((), ())), preferred_element_type=F32)


def both(a, b):
    return (a.astype(F32) + b.astype(F32)).astype(BF16)


def offset(q):
    return jnp.where(q == 0, 2, jnp.where(q == 1, 1, jnp.where(q == 2, 3, 0)))


def kernel(
    rate_ref, hid, cot, wall,
    dx_out, dq_out, dk_out, dv_out,
    X, W, C, QKV, G, GT, PX, RB, EZ, FU, FD, SU, SD, EX, FIN, RFIN,
    DW, YFU, YFD, YSU, YSD, HB0, HB1, RT, PR, inner, qdec, kdec, sdec, fstate, bstate,
    ss, rs, csend, crecv, lsem,
):
    depth = wall.shape[0]
    hd = wall.shape[1] // 3
    s = lax.axis_index("sp")
    d = lax.axis_index("dp")
    z, x = s // 4, s % 4
    y, c = d // 2, d % 2
    g = x // 2
    r = (c + g) % 2
    xp = x + 1 - 2 * (x % 2)
    j = z * 2 + x % 2
    up, down, far = (z + 1) % 4, (z + 3) % 4, (z + 2) % 4
    yu, yd, yf = (y + 1) % 4, (y + 3) % 4, (y + 2) % 4

    def at(zz, xx):
        return zz * 2 + xx % 2

    def dev(sp, dp):
        return {"sp": sp, "dp": dp}

    pair = dev(z * 4 + xp, d)
    zup, zdown = dev(up * 4 + x, d), dev(down * 4 + x, d)
    yup, ydown = dev(s, yu * 2 + c), dev(s, yd * 2 + c)
    sibling = dev(s, y * 2 + 1 - c)
    swap = z * 4 + 3 - x
    copies = {}

    def add(name, src, dst, device, landing=None):
        n = len(copies)
        copies[name] = pltpu.make_async_remote_copy(
            src_ref=src, dst_ref=dst, send_sem=ss.at[n], recv_sem=rs.at[n if landing is None else landing],
            device_id=device, device_id_type=pl.DeviceIdType.MESH,
        )

    def start(*names):
        for name in names:
            copies[name].start()

    def arrived(*names):
        for name in names:
            copies[name].wait_recv()

    half = BLOCK // 2
    quarter = BLOCK // 4
    xr, zr = pl.ds(0, half), pl.ds(half, half)

    def blk(zz, xx, rows):
        return X.at[8 * r + at(zz, xx), rows]

    def ring(name, device, src):
        add(name, src, src, device)

    for n, rows in enumerate((xr, zr)):
        add("swap_x%d" % n, hid.at[0, rows], X.at[8 + at(z, 3 - x), rows], dev(swap, y * 2 + 1 - c))
    ring("A", pair, blk(z, x, xr))
    for tag, xx, rows, o in (("z", x, zr, half), ("a", x, xr, 0), ("b", xp, xr, 0)):
        ring(tag + "u", zup, blk(z, xx, rows))
        ring(tag + "d", zdown, blk(z, xx, rows))
        ring(tag + "uu", zup, blk(down, xx, pl.ds(o, quarter)))
        ring(tag + "dd", zdown, blk(up, xx, pl.ds(o + quarter, quarter)))
    for tag, zz in (("H0", z), ("H1", down), ("H2", up), ("H3", far)):
        ring(tag, pair, blk(zz, x, zr))
    order = [(z, x), (down, x), (up, x), (far, x), (z, xp), (down, xp), (up, xp), (far, xp)]
    for n, (zz, xx) in enumerate(order):
        slot = X.at[8 * r + at(zz, xx)]
        add("D%d" % n, slot, slot, sibling)

    add("own_w", wall, W.at[d], sibling)
    add("swap_w", wall, W.at[d], dev(swap, y * 2 + g), COPIES + c)
    for i in range(2):
        ring("wu%d" % i, yup, W.at[2 * y + i])
        ring("wd%d" % i, ydown, W.at[2 * y + i])
    ring("wuu", yup, W.at[2 * yd])
    ring("wdd", ydown, W.at[2 * yu + 1])
    add("rate", RT, PR, dev(swap, d))

    def out(zz, xx, rows):
        return RB.at[at(zz, xx), rows]

    zorder = (far, up, down, z)
    for n, zz in enumerate(zorder):
        add("P%d" % n, PX.at[pl.ds(8 * (1 - r) + 2 * zz, 2)], RB.at[pl.ds(2 * zz, 2)], sibling)
    for n, zz in enumerate((far, up, down, z)):
        add("EZ%d" % n, out(zz, xp, zr), EZ.at[zz], pair)
    cols3 = ((0, x, 0), (1, xp, 0), (2, x, half))
    for m, xx, o in cols3:
        add("FU%d" % m, out(far, xx, pl.ds(o, quarter)), FU.at[m], zup)
        add("FD%d" % m, out(far, xx, pl.ds(o + quarter, quarter)), FD.at[m], zdown)
        add("SU%d" % m, out(up, xx, pl.ds(o, half)), SU.at[m], zup)
        add("SD%d" % m, out(down, xx, pl.ds(o, half)), SD.at[m], zdown)
    add("EX", out(z, xp, xr), EX, pair)
    for n, rows in enumerate((xr, zr)):
        add("fin%d" % n, FIN.at[rows], RFIN.at[rows], dev(swap, y * 2 + 1 - c))

    for n in range(3):
        add("YFU_%d" % n, DW.at[n, 2 * yf], YFU.at[n], yup)
        add("YFD_%d" % n, DW.at[n, 2 * yf + 1], YFD.at[n], ydown)
        for i in range(2):
            add("YSU%d_%d" % (i, n), DW.at[n, 2 * yu + i], YSU.at[n, i], yup)
            add("YSD%d_%d" % (i, n), DW.at[n, 2 * yd + i], YSD.at[n, i], ydown)
            add("hb1_%d_%d" % (i, n), DW.at[n, 2 * y + i], HB1.at[n], dev(swap, 2 * y + i), COPIES + 2 + n)
        add("hb0_%d" % n, DW.at[n, 2 * y + 1 - c], HB0.at[n], sibling)

    def parts(name):
        return tuple("%s_%d" % (name, n) for n in range(3))

    barrier = pltpu.get_barrier_semaphore()

    def greet(k, _):
        pl.semaphore_signal(
            barrier, inc=1, device_id=dev((s + k // 2) % 16, 2 * y + (c + k) % 2),
            device_id_type=pl.DeviceIdType.MESH,
        )
        return 0

    for device in (yup, ydown):
        pl.semaphore_signal(barrier, inc=1, device_id=device, device_id_type=pl.DeviceIdType.MESH)
    lax.fori_loop(1, 32, greet, 0)

    local_weights = pltpu.make_async_copy(wall, W.at[d], lsem)

    @pl.when(r == 0)
    def _():
        for n, rows in enumerate((xr, zr)):
            pltpu.make_async_copy(hid.at[0, rows], X.at[j, rows], rs.at[n]).start()
        local_weights.start()

    RT[...] = jnp.full(RT.shape, rate_ref[0], F32)
    pl.semaphore_wait(barrier, 33)

    bx = x + r * (3 - 2 * x)
    cslot = 8 * r + z * 2 + bx - 2 * c

    def cot_copy(k):
        h = (s + k) % 16
        hz, hx = h // 4, h % 4
        role = (hx // 2 + c) % 2
        tx = hx + role * (3 - 2 * hx)
        tc = c + role * (1 - 2 * c)
        src = cot.at[0, :, pl.ds(pl.multiple_of(h * hd, hd), hd)]
        same = jnp.logical_and(r == 0, k == 0)
        return same, src, dev(hz * 4 + tx, 2 * y + tc), csend

    def cot_send(k, _):
        same, src, device, sem = cot_copy(k)

        @pl.when(same)
        def _():
            pltpu.make_async_copy(src, C.at[cslot], crecv).start()

        @pl.when(jnp.logical_not(same))
        def _():
            pltpu.make_async_remote_copy(
                src_ref=src, dst_ref=C.at[cslot], send_sem=sem, recv_sem=crecv,
                device_id=device, device_id_type=pl.DeviceIdType.MESH,
            ).start()

        return 0

    def wait_own(n, rows):
        own = X.at[8 * r + j, rows]
        pltpu.make_async_copy(own, own, rs.at[n]).wait()

    def late_a():
        arrived("H1")
        start("D5")
        arrived("H2")
        start("D6")

    def late_b():
        arrived("buu", "bdd", "H3")
        start("D7")

    @pl.when(r == 1)
    def _():
        start("swap_x0", "swap_x1")
        start("own_w")

    wait_own(0, xr)
    start("A", "au", "ad")

    @pl.when(r == 1)
    def _():
        start("swap_w")

    wait_own(1, zr)
    start("zu", "zd", "H0", "D0")

    @pl.when(r == 0)
    def _():
        local_weights.wait()
        arrived("own_w")
        start("wu0", "wd1", "wu1", "wd0")

    start("rate")
    arrived("A")
    start("bu", "bd")

    @pl.when(r == 0)
    def _():
        start("swap_w")

    @pl.when(r == 1)
    def _():
        for i in range(2):
            piece = W.at[2 * y + i]
            pltpu.make_async_copy(piece, piece, rs.at[COPIES + i]).wait()
        start("wu0", "wd1", "wu1", "wd0")

    arrived("au")
    start("auu")
    arrived("ad")
    start("add")
    arrived("zu")
    start("zuu", "H1", "D1")
    arrived("zd")
    start("zdd", "H2", "D2")

    def forward_weights():
        arrived("wu0")
        start("wuu")
        arrived("wd1")
        start("wdd")

    forward_weights()

    @pl.when(r == 1)
    def _():
        lax.fori_loop(0, 16, cot_send, 0)

    arrived("bu")
    start("buu")
    arrived("bd")
    start("bdd")
    arrived("zuu", "zdd")
    start("H3")

    @pl.when(r == 0)
    def _():
        lax.fori_loop(0, 16, cot_send, 0)

    arrived("auu", "add")
    start("D3")
    arrived("H0")
    start("D4")

    @pl.when(r == 0)
    def _():
        late_a()
        late_b()

    arrived("wu1", "wd0", "wuu", "wdd")

    def project(k, _):
        @pl.when(jnp.logical_and(r == 1, k == 4))
        def _():
            late_a()

        @pl.when(jnp.logical_and(r == 1, k == 6))
        def _():
            late_b()

        for n in range(4):

            @pl.when(k == n + 4 * (1 - r))
            def _():
                arrived("D%d" % n, "D%d" % (n + 4))

        q = k % 4
        zz = (z + jnp.where(q == 0, 0, jnp.where(q == 1, 3, jnp.where(q == 2, 1, 2)))) % 4
        rows = pl.ds(8 * (k // 4) + 2 * zz, 2)
        a = X[rows].reshape(2 * BLOCK, X.shape[2])
        for n in range(3):
            b = W[:, :, n * hd : (n + 1) * hd].reshape(X.shape[2], hd)
            QKV[rows, :, n * hd : (n + 1) * hd] = dot(a, b, (1, 0)).astype(BF16).reshape(2, BLOCK, hd)
        return 0

    lax.fori_loop(0, 8, project, 0)

    arrived("rate")
    pltpu.make_async_copy(C, C, crecv).wait()
    rate = jnp.where(r == 0, RT[0:1, :], PR[0:1, :])
    row = lax.broadcasted_iota(jnp.int32, (BLOCK, BLOCK), 0).astype(F32)
    col = lax.broadcasted_iota(jnp.int32, (BLOCK, BLOCK), 1).astype(F32)
    spread = row - col
    inner[...] = jnp.where(spread >= 0, jnp.exp(rate * jnp.maximum(spread, 0.0)), 0.0)
    qd = jnp.exp(rate * (row + 1.0))
    kd = jnp.exp(rate * (BLOCK - 1.0 - row))
    qdec[...] = jnp.concatenate((qd, qd), axis=1)
    kdec[...] = jnp.concatenate((kd, kd), axis=1)
    sd = jnp.exp(rate * float(BLOCK))
    sdec[...] = jnp.concatenate((sd, sd), axis=1)
    fstate[...] = jnp.zeros_like(fstate)
    bstate[...] = jnp.zeros_like(bstate)
    scale = hd ** (-0.5)
    blocks = X.shape[0]

    def load(n):
        px = n % 4
        role = (px // 2 + g) % 2
        slot = 8 * role + at(n // 4, px + role * (3 - 2 * px))
        q = QKV[slot, :, 0:hd]
        k = (QKV[slot, :, hd : 2 * hd].astype(F32) * scale).astype(BF16)
        v = QKV[slot, :, 2 * hd : 3 * hd]
        return slot, q, k, v, C[slot]

    def put(slot, n, value):
        value = value.astype(BF16)
        G[slot, :, n * hd : (n + 1) * hd] = value
        lanes = pl.ds(pl.multiple_of(slot * BLOCK, BLOCK), BLOCK)
        GT[n * hd : (n + 1) * hd, lanes] = value.T

    def retain(i, _):
        slot, q, k, v, ct = load(i)
        mixed = (dot(ct, v, (1, 1)) * inner[...]).astype(BF16)
        st = fstate[...]
        put(slot, 0, dot(mixed, k, (1, 0)) + dot(ct, st.astype(BF16), (1, 0)) * qdec[...])
        kw = (k.astype(F32) * kdec[...]).astype(BF16)
        fstate[...] = st * sdec[...] + dot(v, kw, (0, 0))

        slot, q, k, v, ct = load(blocks - 1 - i)
        mixed = (dot(ct, v, (1, 1)) * inner[...]).astype(BF16)
        scores = (dot(q, k, (1, 1)) * inner[...]).astype(BF16)
        st = bstate[...]
        sb = st.astype(BF16)
        put(slot, 1, (dot(mixed, q, (0, 0)) + dot(v, sb, (1, 1)) * kdec[...]) * scale)
        put(slot, 2, dot(scores, ct, (0, 0)) + dot(k, sb, (1, 0)) * kdec[...])
        qw = (q.astype(F32) * qdec[...]).astype(BF16)
        bstate[...] = st * sdec[...] + dot(qw, ct, (0, 0))
        return 0

    lax.fori_loop(0, blocks, retain, 0)

    def chip_sum(n):
        zz = zorder[n]
        arrived("P%d" % n)
        for xx, names in ((xp, ("EZ%d" % n, "FU1", "FD1")), (x, ("FU0", "FD0"))):
            jj = at(zz, xx)
            RB[jj] = both(RB[jj], PX[8 * r + jj])
            if n:
                names = tuple(name for name in names if name[0] == "E")
            start(*names)

    def merge(ref, index, rows, other):
        ref[index, rows] = both(ref[index, rows], other)

    def ring_up(m):
        _, xx, o = cols3[m]
        arrived("FU%d" % m)
        merge(RB, at(up, xx), pl.ds(o, quarter), FU[m])
        start("SU%d" % m)

    def ring_down(m):
        _, xx, o = cols3[m]
        arrived("FD%d" % m)
        merge(RB, at(down, xx), pl.ds(o + quarter, quarter), FD[m])
        start("SD%d" % m)

    def pair_in(n):
        zz = (far, up, down, z)[n]
        arrived("EZ%d" % n)
        merge(RB, at(zz, x), zr, EZ[zz])

    def yblock(k):
        yo = jnp.where(k < 2, 2, jnp.where(k < 6, jnp.where(k % 2 == 0, 1, 3), 0))
        i = jnp.where(jnp.logical_or(k == 2, k == 3), (k + 1) % 2, k % 2)
        return 2 * ((y + yo) % 4) + i

    def weights_product(k):
        db = yblock(k)
        cols = pl.ds(pl.multiple_of(db * depth, depth), depth)
        b = X[:, :, cols].reshape(blocks * BLOCK, depth)
        for n in range(3):
            part = pl.ds(n * hd, hd)
            DW[n, db] = dot(GT[part, :], b, (1, 0)).astype(BF16)

    def input_product(k, role):
        zz = (z + offset(k)) % 4
        rows = pl.ds(8 * role + 2 * zz, 2)
        a = G[rows].reshape(2 * BLOCK, 3 * hd)
        for n in range(8):
            piece = dot(a, W[n], (1, 1)).astype(BF16)
            PX[rows, :, n * depth : (n + 1) * depth] = piece.reshape(2, BLOCK, depth)

    def products(k, _):
        input_product(k, 1 - r)
        for n in range(4):

            @pl.when(k == n)
            def _():
                start("P%d" % n)

        input_product(k, r)
        weights_product(2 * k)
        for n, names in enumerate((parts("YFU"), parts("YSU1"))):

            @pl.when(k == n)
            def _():
                start(*names)

        for n in range(4):

            @pl.when(k == n)
            def _():
                chip_sum(n)

        @pl.when(k == 2)
        def _():
            ring_up(1)
            ring_down(1)
            pair_in(0)
            start("FU2", "FD2")
            ring_up(0)
            for n in range(3):
                arrived("YFU_%d" % n)
                DW[n, 2 * yu] = both(DW[n, 2 * yu], YFU[n])
                start("YSU0_%d" % n)

        weights_product(2 * k + 1)
        for n, names in enumerate((parts("YFD"), parts("YSD0"))):

            @pl.when(k == n)
            def _():
                start(*names)

        @pl.when(k == 2)
        def _():
            ring_down(0)
            for n in range(3):
                arrived("YFD_%d" % n)
                DW[n, 2 * yd + 1] = both(DW[n, 2 * yd + 1], YFD[n])
                start("YSD1_%d" % n)

        return 0

    lax.fori_loop(0, 4, products, 0)

    def weight_sums(n):
        for i in range(2):
            arrived("YSU%d_%d" % (i, n), "YSD%d_%d" % (i, n))
            total = DW[n, 2 * y + i].astype(F32) + YSU[n, i].astype(F32) + YSD[n, i].astype(F32)
            DW[n, 2 * y + i] = total.astype(BF16)

        @pl.when(r == 1)
        def _():
            start("hb1_0_%d" % n, "hb1_1_%d" % n)

        @pl.when(r == 0)
        def _():
            start("hb0_%d" % n)

    jp = at(z, xp)
    arrived("SU1", "SD1")
    RB[jp, xr] = (RB[jp, xr].astype(F32) + SU[1].astype(F32) + SD[1].astype(F32)).astype(BF16)
    start("EX")
    pair_in(1)
    ring_up(2)
    weight_sums(0)
    pair_in(2)
    ring_down(2)
    weight_sums(1)
    weight_sums(2)
    arrived("SU0", "SD0", "EX")
    total = RB[j, xr].astype(F32) + SU[0].astype(F32) + SD[0].astype(F32) + EX[...].astype(F32)
    FIN[xr] = total.astype(BF16)

    @pl.when(r == 1)
    def _():
        start("fin0")

    pair_in(3)
    arrived("SU2", "SD2")
    total = RB[j, zr].astype(F32) + SU[2].astype(F32) + SD[2].astype(F32)
    FIN[zr] = total.astype(BF16)

    @pl.when(r == 0)
    def _():
        dx_out[0] = FIN[...]

    @pl.when(r == 1)
    def _():
        start("fin1")

    for n, ref in enumerate((dq_out, dk_out, dv_out)):
        pltpu.make_async_copy(HB1.at[n], HB1.at[n], rs.at[COPIES + 2 + n]).wait()

        @pl.when(r == 0)
        def _():
            ref[...] = ((DW[n, 2 * y + c].astype(F32) + HB1[n].astype(F32)) * 0.125).T

        @pl.when(r == 1)
        def _():
            arrived("hb0_%d" % n)
            ref[...] = ((HB0[n].astype(F32) + HB1[n].astype(F32)) * 0.125).T

    @pl.when(r == 1)
    def _():
        arrived("fin0", "fin1")
        dx_out[0] = RFIN[...]

    only_one = ("swap_x0", "swap_x1", "own_w", "fin0", "fin1") + parts("hb1_0") + parts("hb1_1")
    for name in copies:
        if name not in only_one and name[:3] != "hb0":
            copies[name].wait_send()

    @pl.when(r == 1)
    def _():
        for name in only_one:
            copies[name].wait_send()

    @pl.when(r == 0)
    def _():
        for name in parts("hb0"):
            copies[name].wait_send()

    for role in range(2):

        @pl.when(r == role)
        def _():
            sent = C.at[pl.ds(0, 15 + role)]
            pltpu.make_async_copy(sent, sent, csend).wait()


def hand_over(*refs):
    n = len(refs) // 2
    pairs = [pltpu.make_async_copy(refs[i], refs[n + i], refs[-1].at[i]) for i in range(n)]
    for copy in pairs:
        copy.start()
    for copy in pairs:
        copy.wait()


def body(hidden_in, mix_cotangent, query_weight, key_weight, value_weight, decay_log):
    model = hidden_in.shape[2]
    depth, hd = query_weight.shape
    ways = model // depth
    slots = 16
    vmem = pltpu.VMEM
    any_space = pl.BlockSpec(memory_space=pl.ANY)
    far_space = pl.BlockSpec(memory_space=pltpu.HBM)
    whole = pl.BlockSpec(memory_space=pltpu.VMEM)
    grad = jax.ShapeDtypeStruct((depth, hd), F32)
    weights = jnp.concatenate((query_weight, key_weight, value_weight), axis=1)
    results = pl.pallas_call(
        kernel,
        out_shape=(jax.ShapeDtypeStruct(hidden_in.shape, BF16), grad, grad, grad),
        in_specs=[pl.BlockSpec(memory_space=pltpu.SMEM)] + [far_space] * 3,
        out_specs=(whole,) * 4,
        scratch_shapes=[
            vmem((slots, BLOCK, model), BF16),
            vmem((ways, depth, 3 * hd), BF16),
            vmem((slots, BLOCK, hd), BF16),
            vmem((slots, BLOCK, 3 * hd), BF16),
            vmem((slots, BLOCK, 3 * hd), BF16),
            vmem((3 * hd, slots * BLOCK), BF16),
            vmem((slots, BLOCK, model), BF16),
            vmem((slots // 2, BLOCK, model), BF16),
            vmem((4, BLOCK // 2, model), BF16),
            vmem((3, BLOCK // 4, model), BF16),
            vmem((3, BLOCK // 4, model), BF16),
            vmem((3, BLOCK // 2, model), BF16),
            vmem((3, BLOCK // 2, model), BF16),
            vmem((BLOCK // 2, model), BF16),
            vmem((BLOCK, model), BF16),
            vmem((BLOCK, model), BF16),
            vmem((3, ways, hd, depth), BF16),
            vmem((3, hd, depth), BF16),
            vmem((3, hd, depth), BF16),
            vmem((3, 2, hd, depth), BF16),
            vmem((3, 2, hd, depth), BF16),
            vmem((3, hd, depth), BF16),
            vmem((3, hd, depth), BF16),
            vmem((8, BLOCK), F32),
            vmem((8, BLOCK), F32),
            vmem((BLOCK, BLOCK), F32),
            vmem((BLOCK, hd), F32),
            vmem((BLOCK, hd), F32),
            vmem((1, hd), F32),
            vmem((hd, hd), F32),
            vmem((hd, hd), F32),
            pltpu.SemaphoreType.DMA((COPIES,)),
            pltpu.SemaphoreType.DMA((COPIES + 5,)),
            pltpu.SemaphoreType.DMA,
            pltpu.SemaphoreType.DMA,
            pltpu.SemaphoreType.DMA,
        ],
        compiler_params=pltpu.CompilerParams(collective_id=0, has_side_effects=True, vmem_limit_bytes=52 * 1024 * 1024),
    )(decay_log, hidden_in, mix_cotangent, weights)
    return pl.pallas_call(
        hand_over,
        out_shape=(jax.ShapeDtypeStruct(hidden_in.shape, BF16), grad, grad, grad),
        in_specs=[any_space] * 4,
        out_specs=(any_space,) * 4,
        scratch_shapes=[pltpu.SemaphoreType.DMA((4,))],
        compiler_params=pltpu.CompilerParams(vmem_limit_bytes=1024 * 1024),
    )(*results)


def solution(mesh):
    placed = (
        P("dp", "sp", None),
        P("dp", "sp", None),
        P("dp", "sp"),
        P("dp", "sp"),
        P("dp", "sp"),
        P("sp"),
    )
    return jax.shard_map(
        body,
        mesh=mesh,
        in_specs=placed,
        out_specs=(P("dp", "sp", None), P("dp", "sp"), P("dp", "sp"), P("dp", "sp")),
        check_vma=False,
    )
```
